32 devices in a mesh: sp: 8 (over z, x), dp: 4 (over y, core).
Axes of the slice: x: 2, y: 2, z: 4, core: 2. Of those that a mesh axis runs over, the one named last changes fastest.
Arguments:
- resid: bfloat16 [4, 1024, 2048], P('dp', 'sp'), may hold values from -6 to 6
- queries: bfloat16 [4, 1024, 2048], P('dp', 'sp'), may hold values from -7 to 7
- keys: bfloat16 [4, 1024, 2048], P('dp', 'sp'), may hold values from -7 to 7
- values: bfloat16 [4, 1024, 2048], P('dp', 'sp'), may hold values from -6 to 6
- forget_cache: float32 [4, 32, 1024], P('dp', 'sp'), may hold values from -131 to 0, as said below
- query_gain: float32 [64], replicated, may hold values from 0.5 to 8
- key_gain: float32 [64], replicated, may hold values from 0.5 to 8
- out_weight: bfloat16 [2048, 2048], P(None, 'dp'), may hold values from -0.125 to 0.125
- norm_gain: float32 [2048], replicated, may hold values from 0.1 to 1.9
- routes: int32 [4, 1024, 2], P('dp', 'sp'), may hold values from 0 to 31, all different within a row; in each aligned block of 128 rows (0 to 127, 128 to 255, ..., all dimensions but the last counted through in order) at most 16 rows name the same one
- group_weight: float32 [4, 1024], P('dp', 'sp'), may hold values from 0.2 to 1
- inner_share: float32 [4, 1024, 2], P('dp', 'sp'), may hold values from 0.1 to 1
- expert_gate: bfloat16 [32, 2048, 1024], P(('sp', 'dp')), may hold values from -0.125 to 0.125
- expert_up: bfloat16 [32, 2048, 1024], P(('sp', 'dp')), may hold values from -0.125 to 0.125
- expert_down: bfloat16 [32, 1024, 2048], P(('sp', 'dp')), may hold values from -0.1875 to 0.1875
Outputs:
- layer_out: bfloat16 [4, 1024, 2048], P('dp', 'sp')
The draws below stay inside these ranges and needn't reach their ends.
Inputs may be any that keep to these rules, and one draw needn't show every extreme that they name: `routes`: each row names 2 different experts; the rows of one device name one expert at most 16 times, a bound that some block reaches. `forget_cache`: along positions each head's values never rise.
All inputs are finite; a program needn't handle non-finite values.
Results may differ from the reference program's by a relative error of at most 0.0095.
The reference program's roundings to bfloat16 on the way count: a program that leaves them out, or rounds other values in their place, can miss the bound.
Values may be sent and summed in bfloat16 or wider, within the bound.
A program may use at most 128 MiB of HBM per device.

```python
import math
import jax
import jax.numpy as jnp
import numpy as np
from jax import lax

D = 2048
HEAD_COUNT = 32
HD = 64
FF = 1024
TOPK = 2
TOK_DEV = 128
SEQUENCE_COUNT = 4
SEQUENCE_LENGTH = 1024
EXPERTS = 32
CAP = 16


def paired_rows(key):
    base = jax.random.fold_in(key, 7)
    key_q, key_k = jax.random.split(base, 2)
    shape = (SEQUENCE_COUNT, SEQUENCE_LENGTH, HEAD_COUNT * HD)
    key_rows = jax.random.truncated_normal(key_k, -6.0, 6.0, shape, jnp.float32)
    query_rows = jax.random.truncated_normal(key_q, -6.0, 6.0, shape, jnp.float32)
    return (query_rows, key_rows)


def draw_queries(key, part):
    return paired_rows(key)[0].astype(jnp.bfloat16)


def draw_keys(key, part):
    return paired_rows(key)[1].astype(jnp.bfloat16)


def draw_query_gain(key, part):
    sub = jax.random.fold_in(key, 11)
    return jax.random.uniform(sub, (HD,), jnp.float32, 0.5, 1.5)


def draw_key_gain(key, part):
    sub = jax.random.fold_in(key, 13)
    return jax.random.uniform(sub, (HD,), jnp.float32, 0.5, 1.5)


def draw_forget_cache(key, part):
    random_keys = jax.random.split(jax.random.fold_in(key, 17), 7)
    order = jax.random.permutation(random_keys[0], HEAD_COUNT)
    slow = order < HEAD_COUNT // 2
    total = jax.random.uniform(random_keys[1], (SEQUENCE_COUNT, HEAD_COUNT), jnp.float32, 0.3, 1.0)
    fast_span = jax.random.uniform(random_keys[2], (SEQUENCE_COUNT, HEAD_COUNT), jnp.float32, 30.0, 100.0)
    rate = jnp.where(slow[None, :], total / SEQUENCE_LENGTH, 1.0 / fast_span)
    blocks = SEQUENCE_LENGTH // TOK_DEV
    factor = jnp.exp(jax.random.uniform(random_keys[3], (SEQUENCE_COUNT, HEAD_COUNT, blocks), jnp.float32, -0.693, 0.693))
    factor = jnp.repeat(factor, TOK_DEV, axis=2)
    rough = jax.random.uniform(random_keys[4], (SEQUENCE_COUNT, HEAD_COUNT, SEQUENCE_LENGTH), jnp.float32, 0.3, 1.7)
    baseline_level = -rate[:, :, None] * factor * rough
    spike_location = jax.random.randint(random_keys[5], (SEQUENCE_COUNT, HEAD_COUNT, 3), 0, SEQUENCE_LENGTH)
    spike_dropped = jnp.log(jax.random.uniform(random_keys[6], (SEQUENCE_COUNT, HEAD_COUNT, 3), jnp.float32, 0.5, 0.8))
    token_offset = jnp.arange(SEQUENCE_LENGTH, dtype=jnp.int32)
    spike_events = jnp.sum(jnp.where(token_offset[None, None, None, :] == spike_location[..., None], spike_dropped[..., None], 0.0), axis=2)
    return jnp.cumsum(baseline_level + spike_events, axis=2)


def level_of(own_key, dims, cuts, smallest, top_value):
    def one(dim, parts):
        heights = jax.random.uniform(jax.random.fold_in(jax.random.fold_in(own_key, 6), dim), (parts,), jnp.float32, smallest / len(cuts), top_value / len(cuts))
        return jnp.repeat(jnp.exp(heights), dims[dim] // parts).reshape((-1,) + (1,) * (len(dims) - dim - 1))

    level = one(*cuts[0])
    for cut in cuts[1:]:
        level = level * one(*cut)
    return level


def shared_out(key, own, number, rows, count, top, bound, lean):
    ranking = jax.random.permutation(key, count)
    packed, ordinary = portions_of(count, rows * top, bound, lean, True), portions_of(count, rows * top, bound, lean, False)
    places = jnp.arange(count)

    def named(tallies, offset_by):
        used = int((tallies > 0).sum())
        fixed = max(1, used // 4)
        moved = fixed + (places - fixed + offset_by * (used - fixed)) % max(1, count - fixed)
        return jnp.zeros((count,), jnp.int32).at[ranking[jnp.where(places < fixed, places, moved)]].set(jnp.asarray(tallies, jnp.int32))

    tallies = jnp.where(number % 4 == 0, named(packed, number // 4), named(ordinary, number - number // 4 - 1))
    mixed = jax.random.permutation(jax.random.fold_in(own, 3), count)
    source_of, receiver = mixed[0:count // 2 * 2:2], mixed[1:count // 2 * 2:2]
    margin = jnp.minimum(tallies[source_of] - 1, bound - tallies[receiver]) // 2
    margin = jnp.where((source_of == ranking[0]) | (receiver == ranking[0]) | (tallies[receiver] == 0), 0, jnp.maximum(margin, 0))
    moved = jax.random.randint(jax.random.fold_in(own, 4), (count // 2,), 0, 1 << 20) % (margin + 1)
    tallies = tallies.at[source_of].add(-moved).at[receiver].add(moved)
    members = jnp.searchsorted(jnp.cumsum(tallies), jnp.arange(rows * top), side="right").astype(jnp.int32)
    listing = members.reshape(top, rows).T
    listing = listing[jax.random.permutation(jax.random.fold_in(own, 1), rows)]
    offset_by = jax.random.randint(jax.random.fold_in(own, 2), (rows, 1), 0, top)
    return jnp.take_along_axis(listing, (jnp.arange(top)[None, :] + offset_by) % top, axis=1)


def portions_of(number_of, total, limit, lean, full):
    loads = [(1 << 20) // math.isqrt(grade ** lean) + 1 for grade in range(1, number_of + 1)]
    largest = limit if full else min(limit, max(-(-total // number_of), total * loads[0] // sum(loads)))
    least = 1 if total - largest >= number_of - 1 else 0
    counts, surplus = [largest] + [least] * (number_of - 1), total - largest - least * (number_of - 1)
    while surplus > 0:
        free = [i for i in range(1, number_of) if counts[i] < largest] or [i for i in range(1, number_of) if counts[i] < limit]
        pool, remaining = sum([loads[i] for i in free]), surplus
        for i in free:
            extra = min(limit - counts[i], max(1, remaining * loads[i] // pool), surplus)
            counts[i] = counts[i] + extra
            surplus = surplus - extra
    return np.array(counts)


def centred(key, dims, width, limit, shards=(), kind=jnp.bfloat16):
    entries = jax.random.normal(key, dims, jnp.float32) * width
    if len(shards) > 0:
        entries = level_of(key, dims, shards, -0.22, 0.18) * entries
    return jnp.clip(entries, min=-limit, max=limit).astype(kind)


def setup_inputs(seed: int = 0) -> dict:
    key_of = jax.random.split(jax.random.key(seed), 16)
    resid = centred(key_of[0], (SEQUENCE_COUNT, SEQUENCE_LENGTH, D), 1.0, 6.0, ((0, 4), (1, 8)))
    queries = draw_queries(jax.random.fold_in(key_of[15], 71), 0)
    keys = draw_keys(jax.random.fold_in(key_of[15], 71), 0)
    values = centred(key_of[3], (SEQUENCE_COUNT, SEQUENCE_LENGTH, HEAD_COUNT * HD), 1.0, 6.0, ((0, 4), (1, 8)))
    forget_cache = draw_forget_cache(jax.random.fold_in(key_of[15], 71), 0)
    query_gain = draw_query_gain(jax.random.fold_in(key_of[15], 71), 0)
    key_gain = draw_key_gain(jax.random.fold_in(key_of[15], 71), 0)
    out_weight = centred(key_of[7], (HEAD_COUNT * HD, D), (HEAD_COUNT * HD) ** -0.5, 0.125, ((1, 4),))
    norm_gain = jnp.clip(1.0 + 0.18 * jax.random.normal(key_of[8], (D,), jnp.float32), 0.1, 1.9)
    routes_keys = jax.random.split(jax.random.fold_in(key_of[9], 1), SEQUENCE_COUNT * SEQUENCE_LENGTH // TOK_DEV)
    routes_turns = jax.random.permutation(jax.random.fold_in(key_of[9], 3), SEQUENCE_COUNT * SEQUENCE_LENGTH // TOK_DEV)
    routes = jax.vmap(lambda own, number: shared_out(jax.random.fold_in(key_of[9], 2), own, number, TOK_DEV, EXPERTS, TOPK, CAP, 2))(routes_keys, routes_turns).reshape((SEQUENCE_COUNT, SEQUENCE_LENGTH, TOPK))
    group_weight = jnp.clip(jnp.exp(math.log(1.0) - 1.609438 * jax.random.uniform(key_of[10], (SEQUENCE_COUNT, SEQUENCE_LENGTH), jnp.float32) ** level_of(key_of[10], (SEQUENCE_COUNT, SEQUENCE_LENGTH), ((0, 4), (1, 8)), -0.2, 0.2)), 0.2, 1.0)
    inner_share = jnp.clip(jnp.exp(math.log(1.0) - 2.3025851 * jax.random.uniform(key_of[11], (SEQUENCE_COUNT, SEQUENCE_LENGTH, TOPK), jnp.float32) ** level_of(key_of[11], (SEQUENCE_COUNT, SEQUENCE_LENGTH, TOPK), ((0, 4), (1, 8)), -0.2, 0.2)), 0.1, 1.0)
    expert_gate = centred(key_of[12], (EXPERTS, D, FF), D ** -0.5, 0.125, ((0, 32),))
    expert_up = centred(key_of[13], (EXPERTS, D, FF), D ** -0.5, 0.125, ((0, 32),))
    expert_down = centred(key_of[14], (EXPERTS, FF, D), FF ** -0.5, 0.1875, ((0, 32),))
    return dict(resid=resid, queries=queries, keys=keys, values=values, forget_cache=forget_cache, query_gain=query_gain, key_gain=key_gain, out_weight=out_weight, norm_gain=norm_gain, routes=routes, group_weight=group_weight, inner_share=inner_share, expert_gate=expert_gate, expert_up=expert_up, expert_down=expert_down)


EPS = 1e-06

def norm_rows(inputs, gain):
    floats = inputs.astype(jnp.float32)
    scaled = floats * lax.rsqrt(lax.optimization_barrier(jnp.mean(floats * floats, axis=-1, keepdims=True)) + EPS)
    return (scaled * gain.astype(jnp.float32)).astype(jnp.bfloat16)

def head_attention(operands):
    query_rows, key_rows, value_rows, decay = operands
    scores = jnp.dot(query_rows, key_rows.T, preferred_element_type=jnp.float32) * HD ** (-0.5)
    scores = scores + decay[:, None] - decay[None, :]
    token_offset = jnp.arange(query_rows.shape[0], dtype=jnp.int32)
    scores = jnp.where(token_offset[None, :] <= token_offset[:, None], scores, -jnp.inf)
    highest = lax.optimization_barrier(jnp.max(scores, axis=-1, keepdims=True))
    expd = jnp.exp(scores - highest)
    probs = (expd / lax.optimization_barrier(jnp.sum(expd, axis=-1, keepdims=True))).astype(jnp.bfloat16)
    return jnp.dot(probs, value_rows, preferred_element_type=jnp.float32).astype(jnp.bfloat16)

def reference(resid, queries, keys, values, forget_cache, query_gain, key_gain, out_weight, norm_gain, routes, group_weight, inner_share, expert_gate, expert_up, expert_down):

    def sequence_attention(operands):
        seq_q, seq_k, seq_v, seq_c = operands
        query_normed = norm_rows(seq_q.reshape(SEQUENCE_LENGTH, HEAD_COUNT, HD), query_gain).transpose(1, 0, 2)
        key_normed = norm_rows(seq_k.reshape(SEQUENCE_LENGTH, HEAD_COUNT, HD), key_gain).transpose(1, 0, 2)
        value_heads = seq_v.reshape(SEQUENCE_LENGTH, HEAD_COUNT, HD).transpose(1, 0, 2)
        outputs = lax.map(head_attention, (query_normed, key_normed, value_heads, seq_c))
        return outputs.transpose(1, 0, 2).reshape(SEQUENCE_LENGTH, HEAD_COUNT * HD)
    attn = lax.map(sequence_attention, (queries, keys, values, forget_cache))
    projected = jnp.dot(attn.reshape(-1, HEAD_COUNT * HD), out_weight, preferred_element_type=jnp.float32)
    mid = (resid.reshape(-1, D).astype(jnp.float32) + projected).astype(jnp.bfloat16)
    normed = norm_rows(mid, norm_gain)
    shares = inner_share.reshape(-1, TOPK).astype(jnp.float32)
    weights = group_weight.reshape(-1, 1).astype(jnp.float32) * shares / lax.optimization_barrier(jnp.sum(shares, axis=-1, keepdims=True))
    flat_weights = weights.reshape(-1)
    flat_routes = routes.reshape(-1).astype(jnp.int32)
    slot_count = EXPERTS * CAP
    slot_place = jnp.arange(slot_count, dtype=jnp.int32)

    def one_expert(total, expert_index):
        hit = flat_routes == expert_index
        hit_count = jnp.sum(hit.astype(jnp.int32))
        picked = jnp.nonzero(hit, size=slot_count, fill_value=0)[0].astype(jnp.int32)
        live = slot_place < hit_count
        token_index = (picked // TOPK).astype(jnp.int32)
        rows = normed[token_index]
        gate = jnp.dot(rows, expert_gate[expert_index], preferred_element_type=jnp.float32)
        upper = jnp.dot(rows, expert_up[expert_index], preferred_element_type=jnp.float32)
        hidden = (jax.nn.silu(gate) * upper).astype(jnp.bfloat16)
        result = jnp.dot(hidden, expert_down[expert_index], preferred_element_type=jnp.float32).astype(jnp.bfloat16)
        scale = jnp.where(live, flat_weights[picked], jnp.zeros_like(flat_weights[picked]))
        total = total.at[token_index].add(result.astype(jnp.float32) * scale[:, None])
        return (total, None)
    start = jnp.zeros((mid.shape[0], D), jnp.float32)
    mixed, _ = lax.scan(one_expert, start, jnp.arange(EXPERTS, dtype=jnp.int32))
    layer_out = (mid.astype(jnp.float32) + mixed).astype(jnp.bfloat16)
    return layer_out.reshape(SEQUENCE_COUNT, SEQUENCE_LENGTH, D)
```

```python
import functools

import jax
import jax.numpy as jnp
from jax import lax
from jax.experimental import pallas as pl
from jax.experimental.pallas import tpu as pltpu
from jax.sharding import PartitionSpec as P

EPS = 1e-06


def norm_rows(inputs, gain):
    floats = inputs.astype(jnp.float32)
    scaled = floats * lax.rsqrt(jnp.mean(floats * floats, axis=-1, keepdims=True) + EPS)
    return (scaled * gain).astype(jnp.bfloat16)


MESH = pl.DeviceIdType.MESH
LANES = 128
BLOCK = 256


def place(index, size):
    return pl.ds(pl.multiple_of(index * size, size), size)


def half_means(squares, head_size):
    lane = lax.broadcasted_iota(jnp.int32, (LANES, LANES), 0) // head_size
    other = lax.broadcasted_iota(jnp.int32, (LANES, LANES), 1) // head_size
    same = (lane == other).astype(jnp.float32).astype(jnp.bfloat16)
    high = squares.astype(jnp.bfloat16)
    low = (squares - high.astype(jnp.float32)).astype(jnp.bfloat16)
    total = jnp.dot(high, same, preferred_element_type=jnp.float32)
    total = total + jnp.dot(low, same, preferred_element_type=jnp.float32)
    return total * (1.0 / head_size)


def attention_kernel(
    n, head_size,
    q_ref, k_ref, v_ref, decay_ref, q_gain_ref, k_gain_ref,
    out_ref,
    q_buf, k_buf, v_buf, q_norm, k_head, v_ones, o_buf,
    local_sem, send_sem, recv_sem, own_sem, back_send, back_recv,
):
    me = lax.axis_index("sp")
    tok = q_ref.shape[0]
    pairs, length = q_buf.shape[0], q_buf.shape[1]
    inner = LANES // head_size
    sources, buffers = (q_ref, k_ref, v_ref), (q_buf, k_buf, v_buf)

    barrier = pltpu.get_barrier_semaphore()
    for step in range(1, n):
        pl.semaphore_signal(
            barrier, inc=1, device_id={"sp": lax.rem(me + step, n)}, device_id_type=MESH
        )
    pl.semaphore_wait(barrier, n - 1)

    def outgoing(kind, pair, step):
        target = lax.rem(me + step, n)
        return pltpu.make_async_remote_copy(
            src_ref=sources[kind].at[:, place(target * pairs + pair, LANES)],
            dst_ref=buffers[kind].at[pair, place(me, tok), :],
            send_sem=send_sem.at[kind, pair, step],
            recv_sem=recv_sem.at[kind, pair, step],
            device_id={"sp": target},
            device_id_type=MESH,
        )

    def own(kind, pair):
        return pltpu.make_async_copy(
            sources[kind].at[:, place(me * pairs + pair, LANES)],
            buffers[kind].at[pair, place(me, tok), :],
            local_sem.at[kind, pair],
        )

    def backward(pair, step):
        target = lax.rem(me + step, n)
        return pltpu.make_async_remote_copy(
            src_ref=o_buf.at[pair, place(target, tok), :],
            dst_ref=out_ref.at[:, place(me * pairs + pair, LANES)],
            send_sem=back_send.at[pair, step],
            recv_sem=back_recv.at[pair, step],
            device_id={"sp": target},
            device_id_type=MESH,
        )

    def own_back(pair):
        return pltpu.make_async_copy(
            o_buf.at[pair, place(me, tok), :],
            out_ref.at[:, place(me * pairs + pair, LANES)],
            own_sem.at[pair],
        )

    for pair in range(pairs):
        for step in range(1, n):
            for kind in range(3):
                outgoing(kind, pair, step).start()
        for kind in range(3):
            own(kind, pair).start()

    row = lax.broadcasted_iota(jnp.int32, (BLOCK, BLOCK), 0)
    col = lax.broadcasted_iota(jnp.int32, (BLOCK, BLOCK), 1)
    lane = lax.broadcasted_iota(jnp.int32, (length, LANES), 1) // head_size
    out_lane = lax.broadcasted_iota(jnp.int32, (BLOCK, LANES), 1) // head_size
    scale = head_size ** (-0.5)
    v_ones[:, LANES:] = jnp.ones((length, LANES), jnp.bfloat16)

    def scores_of(queries, keys):
        return lax.dot_general(
            queries, keys, (((1,), (1,)), ((), ())), preferred_element_type=jnp.float32
        )

    def one_pair(pair, carry):
        for kind in range(3):
            own(kind, pair).wait()
            for step in range(1, n):
                outgoing(kind, pair, step).wait_recv()
        floats = q_buf[pair].astype(jnp.float32)
        floats = floats * lax.rsqrt(half_means(floats * floats, head_size) + EPS)
        normed = (floats * q_gain_ref[...]).astype(jnp.bfloat16)
        q_norm[...] = (normed.astype(jnp.float32) * scale).astype(jnp.bfloat16)
        floats = k_buf[pair].astype(jnp.float32)
        floats = floats * lax.rsqrt(half_means(floats * floats, head_size) + EPS)
        floats = floats * k_gain_ref[...]
        for head in range(inner):
            k_head[head] = jnp.where(lane == head, floats, 0.0).astype(jnp.bfloat16)
        v_ones[:, :LANES] = v_buf[pair]
        for block in range(length // BLOCK):
            first = block * BLOCK
            here = slice(first, first + BLOCK)
            query_block = q_norm[here, :]
            merged = None
            for head in range(inner):
                decay = decay_ref[pl.ds(pair * inner + head, 1), :]
                decay_here = decay[:, here]
                query_decay = jnp.sum(
                    jnp.where(row == col, decay_here, 0.0), axis=1, keepdims=True
                )
                near = scores_of(query_block, k_head[head, here, :])
                near = near + (query_decay - decay_here)
                near = jnp.where(col <= row, near, -jnp.inf)
                highest = jnp.max(near, axis=1, keepdims=True)
                if block > 0:
                    far = scores_of(query_block, k_head[head, :first, :])
                    far = far + (query_decay - decay[:, :first])
                    highest = jnp.maximum(highest, jnp.max(far, axis=1, keepdims=True))
                total = jnp.dot(
                    jnp.exp(near - highest).astype(jnp.bfloat16),
                    v_ones[here, :],
                    preferred_element_type=jnp.float32,
                )
                if block > 0:
                    total = total + jnp.dot(
                        jnp.exp(far - highest).astype(jnp.bfloat16),
                        v_ones[:first, :],
                        preferred_element_type=jnp.float32,
                    )
                result = total[:, :LANES] / total[:, LANES:]
                merged = result if head == 0 else jnp.where(out_lane == head, result, merged)
            o_buf[pair, here, :] = merged.astype(jnp.bfloat16)
        for step in range(1, n):
            backward(pair, step).start()
        own_back(pair).start()
        return carry

    lax.fori_loop(0, pairs, one_pair, 0)

    def finish(pair, carry):
        own_back(pair).wait()
        for step in range(1, n):
            backward(pair, step).wait()
            for kind in range(3):
                outgoing(kind, pair, step).wait_send()
        return carry

    lax.fori_loop(0, pairs, finish, 0)


def exchange_attention(queries, keys, values, decay, query_gain, key_gain):
    tok, width = queries.shape
    n = lax.axis_size("sp")
    head_size = query_gain.shape[0]
    inner = LANES // head_size
    pairs = width // n // LANES
    length = n * tok
    return pl.pallas_call(
        functools.partial(attention_kernel, n, head_size),
        out_shape=jax.ShapeDtypeStruct((tok, width), jnp.bfloat16),
        in_specs=[pl.BlockSpec(memory_space=pltpu.VMEM)] * 6,
        out_specs=pl.BlockSpec(memory_space=pltpu.VMEM),
        scratch_shapes=[
            pltpu.VMEM((pairs, length, LANES), jnp.bfloat16),
            pltpu.VMEM((pairs, length, LANES), jnp.bfloat16),
            pltpu.VMEM((pairs, length, LANES), jnp.bfloat16),
            pltpu.VMEM((length, LANES), jnp.bfloat16),
            pltpu.VMEM((inner, length, LANES), jnp.bfloat16),
            pltpu.VMEM((length, 2 * LANES), jnp.bfloat16),
            pltpu.VMEM((pairs, length, LANES), jnp.bfloat16),
            pltpu.SemaphoreType.DMA((3, pairs)),
            pltpu.SemaphoreType.DMA((3, pairs, n)),
            pltpu.SemaphoreType.DMA((3, pairs, n)),
            pltpu.SemaphoreType.DMA((pairs,)),
            pltpu.SemaphoreType.DMA((pairs, n)),
            pltpu.SemaphoreType.DMA((pairs, n)),
        ],
        compiler_params=pltpu.CompilerParams(
            collective_id=0, has_side_effects=True, vmem_limit_bytes=40 * 1024 * 1024
        ),
        name="attention",
    )(
        queries, keys, values, decay,
        jnp.tile(query_gain, inner)[None, :], jnp.tile(key_gain, inner)[None, :],
    )


def expert_kernel(
    sp_size, dp_size, per,
    send_ref, gate_ref, up_ref, down_ref,
    out_ref,
    arrived, result, gate_buf, up_buf, down_buf,
    weight_sem, send_sem, recv_sem, back_send, back_recv,
):
    n = sp_size * dp_size
    me = lax.axis_index("sp") * dp_size + lax.axis_index("dp")
    cap, width = send_ref.shape[1], send_ref.shape[2]
    loads = [
        pltpu.make_async_copy(source, target, weight_sem.at[index])
        for index, (source, target) in enumerate(
            ((gate_ref, gate_buf), (up_ref, up_buf), (down_ref, down_buf))
        )
    ]
    for load in loads:
        load.start()

    def coords(flat):
        return {"sp": flat // dp_size, "dp": flat % dp_size}

    barrier = pltpu.get_barrier_semaphore()

    def greet(step, carry):
        pl.semaphore_signal(
            barrier, inc=1, device_id=coords((me + step) % n), device_id_type=MESH
        )
        return carry

    lax.fori_loop(1, n, greet, 0)
    pl.semaphore_wait(barrier, n - 1)

    def outgoing(step):
        target = (me + step) % n
        return pltpu.make_async_remote_copy(
            src_ref=send_ref.at[target],
            dst_ref=arrived.at[step],
            send_sem=send_sem.at[step],
            recv_sem=recv_sem.at[step],
            device_id=coords(target),
            device_id_type=MESH,
        )

    def backward(step):
        target = (me + n - step) % n
        return pltpu.make_async_remote_copy(
            src_ref=result.at[step],
            dst_ref=out_ref.at[me],
            send_sem=back_send.at[step],
            recv_sem=back_recv.at[step],
            device_id=coords(target),
            device_id_type=MESH,
        )

    own = pltpu.make_async_copy(send_ref.at[me], arrived.at[0], recv_sem.at[0])
    own_back = pltpu.make_async_copy(result.at[0], out_ref.at[me], back_recv.at[0])

    def launch(step, carry):
        outgoing(step).start()
        return carry

    lax.fori_loop(1, n, launch, 0)
    own.start()
    for load in loads:
        load.wait()

    def chunk(index, carry):
        first = index * per
        for offset in range(per):
            if offset == 0:
                @pl.when(index == 0)
                def _():
                    own.wait()

                @pl.when(index > 0)
                def _():
                    outgoing(first).wait_recv()
            else:
                outgoing(first + offset).wait_recv()
        rows = arrived[pl.ds(first, per)].reshape(per * cap, width)
        gate = jnp.dot(rows, gate_buf[...], preferred_element_type=jnp.float32)
        upper = jnp.dot(rows, up_buf[...], preferred_element_type=jnp.float32)
        hidden = (gate / (1.0 + jnp.exp(-gate)) * upper).astype(jnp.bfloat16)
        product = jnp.dot(hidden, down_buf[...], preferred_element_type=jnp.float32)
        result[pl.ds(first, per)] = product.astype(jnp.bfloat16).reshape(per, cap, width)
        for offset in range(per):
            if offset == 0:
                @pl.when(index == 0)
                def _():
                    own_back.start()

                @pl.when(index > 0)
                def _():
                    backward(first).start()
            else:
                backward(first + offset).start()
        return carry

    lax.fori_loop(0, n // per, chunk, 0)

    def finish(step, carry):
        outgoing(step).wait_send()
        backward(step).wait()
        return carry

    own_back.wait()
    lax.fori_loop(1, n, finish, 0)


def run_experts(send, gate, upper, down):
    n, cap, width = send.shape
    sp_size, dp_size = lax.axis_size("sp"), lax.axis_size("dp")
    per = max(1, min(n, LANES // cap))
    return pl.pallas_call(
        functools.partial(expert_kernel, sp_size, dp_size, per),
        out_shape=jax.ShapeDtypeStruct(send.shape, jnp.bfloat16),
        in_specs=[pl.BlockSpec(memory_space=pltpu.VMEM)]
        + [pl.BlockSpec(memory_space=pl.ANY)] * 3,
        out_specs=pl.BlockSpec(memory_space=pltpu.VMEM),
        scratch_shapes=[
            pltpu.VMEM(send.shape, jnp.bfloat16),
            pltpu.VMEM(send.shape, jnp.bfloat16),
            pltpu.VMEM(gate.shape, jnp.bfloat16),
            pltpu.VMEM(upper.shape, jnp.bfloat16),
            pltpu.VMEM(down.shape, jnp.bfloat16),
            pltpu.SemaphoreType.DMA((3,)),
            pltpu.SemaphoreType.DMA((n,)),
            pltpu.SemaphoreType.DMA((n,)),
            pltpu.SemaphoreType.DMA((n,)),
            pltpu.SemaphoreType.DMA((n,)),
        ],
        compiler_params=pltpu.CompilerParams(
            collective_id=1, has_side_effects=True, vmem_limit_bytes=56 * 1024 * 1024
        ),
        name="experts",
    )(send, gate, upper, down)


def shards(
    resid,
    queries,
    keys,
    values,
    forget_cache,
    query_gain,
    key_gain,
    out_weight,
    norm_gain,
    routes,
    group_weight,
    inner_share,
    expert_gate,
    expert_up,
    expert_down,
):
    token_attn = exchange_attention(
        queries[0], keys[0], values[0], forget_cache[0], query_gain, key_gain
    )
    projected = jnp.dot(
        token_attn,
        lax.all_gather(out_weight, "dp", axis=1, tiled=True),
        preferred_element_type=jnp.float32,
    )
    mid = (resid[0].astype(jnp.float32) + projected).astype(jnp.bfloat16)
    normed = norm_rows(mid, norm_gain)
    width = normed.shape[1]
    tok_count = normed.shape[0]
    top_count = routes.shape[2]
    experts = lax.axis_size("sp") * lax.axis_size("dp")
    capacity = 2 * tok_count * top_count // experts
    expert_ids = routes[0].reshape(-1)
    expert_onehot = (expert_ids[:, None] == jnp.arange(experts, dtype=jnp.int32)[None, :]).astype(
        jnp.int32
    )
    earlier = jnp.cumsum(expert_onehot, axis=0) - expert_onehot
    slot_rank = jnp.sum(earlier * expert_onehot, axis=1)
    slot_index = (expert_ids * capacity + slot_rank).reshape(tok_count, top_count)
    slot_range = jnp.arange(experts * capacity, dtype=jnp.int32)
    dispatch = jnp.any(slot_range[:, None, None] == slot_index[None, :, :], axis=2).astype(
        jnp.bfloat16
    )
    send = jnp.dot(dispatch, normed, preferred_element_type=jnp.float32).astype(jnp.bfloat16)
    returned = run_experts(
        send.reshape(experts, capacity, width), expert_gate[0], expert_up[0], expert_down[0]
    )
    returned = returned.reshape(experts * capacity, width)
    shares = inner_share[0]
    weights = group_weight[0][:, None] * shares / jnp.sum(shares, axis=-1, keepdims=True)
    mixed = jnp.zeros((tok_count, width), jnp.float32)
    for route in range(top_count):
        select = (slot_range[None, :] == slot_index[:, route : route + 1]).astype(jnp.bfloat16)
        picked = jnp.dot(select, returned, preferred_element_type=jnp.float32)
        mixed = mixed + weights[:, route : route + 1] * picked
    layer_out = (mid.astype(jnp.float32) + mixed).astype(jnp.bfloat16)
    return layer_out.reshape(1, tok_count, width)


def solution(mesh):
    return jax.shard_map(
        shards,
        mesh=mesh,
        in_specs=(
            P("dp", "sp", None),
            P("dp", "sp", None),
            P("dp", "sp", None),
            P("dp", "sp", None),
            P("dp", "sp", None),
            P(),
            P(),
            P(None, "dp"),
            P(),
            P("dp", "sp", None),
            P("dp", "sp"),
            P("dp", "sp", None),
            P(("sp", "dp"), None, None),
            P(("sp", "dp"), None, None),
            P(("sp", "dp"), None, None),
        ),
        out_specs=P("dp", "sp", None),
        check_vma=False,
    )
```

```python
import functools

import jax
import jax.numpy as jnp
from jax import lax
from jax.experimental import pallas as pl
from jax.experimental.pallas import tpu as pltpu
from jax.sharding import PartitionSpec as P

EPS = 1e-06


def norm_rows(inputs, gain):
    floats = inputs.astype(jnp.float32)
    scaled = floats * lax.rsqrt(jnp.mean(floats * floats, axis=-1, keepdims=True) + EPS)
    return (scaled * gain).astype(jnp.bfloat16)


MESH = pl.DeviceIdType.MESH
LANES = 128
BLOCK = 256


def place(index, size):
    return pl.ds(pl.multiple_of(index * size, size), size)


def half_means(squares, head_size):
    lane = lax.broadcasted_iota(jnp.int32, (LANES, LANES), 0) // head_size
    other = lax.broadcasted_iota(jnp.int32, (LANES, LANES), 1) // head_size
    same = (lane == other).astype(jnp.float32).astype(jnp.bfloat16)
    high = squares.astype(jnp.bfloat16)
    low = (squares - high.astype(jnp.float32)).astype(jnp.bfloat16)
    total = jnp.dot(high, same, preferred_element_type=jnp.float32)
    total = total + jnp.dot(low, same, preferred_element_type=jnp.float32)
    return total * (1.0 / head_size)


def attention_kernel(
    n, dp_size, head_size,
    q_ref, k_ref, v_ref, decay_ref, q_gain_ref, k_gain_ref, weight_ref,
    projected_ref, out_ref, weights,
    q_buf, k_buf, v_buf, q_norm, k_head, v_ones, o_buf,
    local_sem, send_sem, recv_sem, own_sem, back_send, back_recv,
    weight_sem, weight_send, weight_recv, pass_send, pass_recv,
):
    me = lax.axis_index("sp")
    column = lax.axis_index("dp")
    rows_y = dp_size // 2
    row_y, core = column // 2, column % 2
    twin = row_y * 2 + 1 - core
    tok = q_ref.shape[0]
    pairs, length = q_buf.shape[0], q_buf.shape[1]
    inner = LANES // head_size
    sources, buffers = (q_ref, k_ref, v_ref), (q_buf, k_buf, v_buf)

    barrier = pltpu.get_barrier_semaphore()
    for step in range(1, n):
        pl.semaphore_signal(
            barrier, inc=1, device_id={"sp": lax.rem(me + step, n)}, device_id_type=MESH
        )
    for step in range(1, rows_y):
        pl.semaphore_signal(
            barrier, inc=1, device_id={"dp": lax.rem(row_y + step, rows_y) * 2 + core},
            device_id_type=MESH,
        )
    pl.semaphore_signal(barrier, inc=1, device_id={"dp": twin}, device_id_type=MESH)
    pl.semaphore_wait(barrier, n - 1 + rows_y)

    def weight_across(step):
        return pltpu.make_async_remote_copy(
            src_ref=weight_ref,
            dst_ref=weights.at[column],
            send_sem=weight_send.at[step],
            recv_sem=weight_recv.at[step],
            device_id={"dp": lax.rem(row_y + step, rows_y) * 2 + core},
            device_id_type=MESH,
        )

    def weight_pass(step):
        block = lax.rem(row_y + rows_y - step, rows_y) * 2 + core
        return pltpu.make_async_remote_copy(
            src_ref=weight_ref if step == 0 else weights.at[block],
            dst_ref=weights.at[block],
            send_sem=pass_send.at[step],
            recv_sem=pass_recv.at[step],
            device_id={"dp": twin},
            device_id_type=MESH,
        )

    weight_own = pltpu.make_async_copy(weight_ref, weights.at[column], weight_sem)

    def outgoing(kind, pair, step):
        target = lax.rem(me + step, n)
        return pltpu.make_async_remote_copy(
            src_ref=sources[kind].at[:, place(target * pairs + pair, LANES)],
            dst_ref=buffers[kind].at[pair, place(me, tok), :],
            send_sem=send_sem.at[kind, pair, step],
            recv_sem=recv_sem.at[kind, pair, step],
            device_id={"sp": target},
            device_id_type=MESH,
        )

    def own(kind, pair):
        return pltpu.make_async_copy(
            sources[kind].at[:, place(me * pairs + pair, LANES)],
            buffers[kind].at[pair, place(me, tok), :],
            local_sem.at[kind, pair],
        )

    def backward(pair, step):
        target = lax.rem(me + step, n)
        return pltpu.make_async_remote_copy(
            src_ref=o_buf.at[pair, place(target, tok), :],
            dst_ref=out_ref.at[:, place(me * pairs + pair, LANES)],
            send_sem=back_send.at[pair, step],
            recv_sem=back_recv.at[pair, step],
            device_id={"sp": target},
            device_id_type=MESH,
        )

    def own_back(pair):
        return pltpu.make_async_copy(
            o_buf.at[pair, place(me, tok), :],
            out_ref.at[:, place(me * pairs + pair, LANES)],
            own_sem.at[pair],
        )

    for pair in range(pairs):
        for step in range(1, n):
            for kind in range(3):
                outgoing(kind, pair, step).start()
        for kind in range(3):
            own(kind, pair).start()

    for step in range(1, rows_y):
        weight_across(step).start()
    weight_pass(0).start()
    weight_own.start()

    row = lax.broadcasted_iota(jnp.int32, (BLOCK, BLOCK), 0)
    col = lax.broadcasted_iota(jnp.int32, (BLOCK, BLOCK), 1)
    lane = lax.broadcasted_iota(jnp.int32, (length, LANES), 1) // head_size
    out_lane = lax.broadcasted_iota(jnp.int32, (BLOCK, LANES), 1) // head_size
    scale = head_size ** (-0.5)
    v_ones[:, LANES:] = jnp.ones((length, LANES), jnp.bfloat16)

    def scores_of(queries, keys):
        return lax.dot_general(
            queries, keys, (((1,), (1,)), ((), ())), preferred_element_type=jnp.float32
        )

    def one_pair(pair, carry):
        for kind in range(3):
            own(kind, pair).wait()
            for step in range(1, n):
                outgoing(kind, pair, step).wait_recv()
        floats = q_buf[pair].astype(jnp.float32)
        floats = floats * lax.rsqrt(half_means(floats * floats, head_size) + EPS)
        normed = (floats * q_gain_ref[...]).astype(jnp.bfloat16)
        q_norm[...] = (normed.astype(jnp.float32) * scale).astype(jnp.bfloat16)
        floats = k_buf[pair].astype(jnp.float32)
        floats = floats * lax.rsqrt(half_means(floats * floats, head_size) + EPS)
        floats = floats * k_gain_ref[...]
        for head in range(inner):
            k_head[head] = jnp.where(lane == head, floats, 0.0).astype(jnp.bfloat16)
        v_ones[:, :LANES] = v_buf[pair]
        for block in range(length // BLOCK):
            first = block * BLOCK
            here = slice(first, first + BLOCK)
            query_block = q_norm[here, :]
            merged = None
            for head in range(inner):
                decay = decay_ref[pl.ds(pair * inner + head, 1), :]
                decay_here = decay[:, here]
                query_decay = jnp.sum(
                    jnp.where(row == col, decay_here, 0.0), axis=1, keepdims=True
                )
                near = scores_of(query_block, k_head[head, here, :])
                near = near + (query_decay - decay_here)
                near = jnp.where(col <= row, near, -jnp.inf)
                highest = jnp.max(near, axis=1, keepdims=True)
                if block > 0:
                    far = scores_of(query_block, k_head[head, :first, :])
                    far = far + (query_decay - decay[:, :first])
                    highest = jnp.maximum(highest, jnp.max(far, axis=1, keepdims=True))
                total = jnp.dot(
                    jnp.exp(near - highest).astype(jnp.bfloat16),
                    v_ones[here, :],
                    preferred_element_type=jnp.float32,
                )
                if block > 0:
                    total = total + jnp.dot(
                        jnp.exp(far - highest).astype(jnp.bfloat16),
                        v_ones[:first, :],
                        preferred_element_type=jnp.float32,
                    )
                result = total[:, :LANES] / total[:, LANES:]
                merged = result if head == 0 else jnp.where(out_lane == head, result, merged)
            o_buf[pair, here, :] = merged.astype(jnp.bfloat16)
        for step in range(1, n):
            backward(pair, step).start()
        own_back(pair).start()
        return carry

    lax.fori_loop(0, pairs, one_pair, 0)
    for step in range(1, rows_y):
        weight_across(step).wait_recv()
        weight_pass(step).start()

    def finish(pair, carry):
        own_back(pair).wait()
        for step in range(1, n):
            backward(pair, step).wait()
            for kind in range(3):
                outgoing(kind, pair, step).wait_send()
        return carry

    lax.fori_loop(0, pairs, finish, 0)
    weight_own.wait()
    for step in range(1, rows_y):
        weight_across(step).wait_send()
    for step in range(rows_y):
        weight_pass(step).wait()
    span = weights.shape[2]
    for block in range(dp_size):
        projected_ref[:, block * span : (block + 1) * span] = jnp.dot(
            out_ref[...], weights[block], preferred_element_type=jnp.float32
        )


def exchange_attention(queries, keys, values, decay, query_gain, key_gain, out_weight):
    tok, width = queries.shape
    n, dp_size = lax.axis_size("sp"), lax.axis_size("dp")
    head_size = query_gain.shape[0]
    inner = LANES // head_size
    pairs = width // n // LANES
    length = n * tok
    return pl.pallas_call(
        functools.partial(attention_kernel, n, dp_size, head_size),
        out_shape=jax.ShapeDtypeStruct((tok, dp_size * out_weight.shape[1]), jnp.float32),
        in_specs=[pl.BlockSpec(memory_space=pltpu.VMEM)] * 6
        + [pl.BlockSpec(memory_space=pl.ANY)],
        out_specs=pl.BlockSpec(memory_space=pltpu.VMEM),
        scratch_shapes=[
            pltpu.VMEM((tok, width), jnp.bfloat16),
            pltpu.VMEM((dp_size,) + out_weight.shape, jnp.bfloat16),
            pltpu.VMEM((pairs, length, LANES), jnp.bfloat16),
            pltpu.VMEM((pairs, length, LANES), jnp.bfloat16),
            pltpu.VMEM((pairs, length, LANES), jnp.bfloat16),
            pltpu.VMEM((length, LANES), jnp.bfloat16),
            pltpu.VMEM((inner, length, LANES), jnp.bfloat16),
            pltpu.VMEM((length, 2 * LANES), jnp.bfloat16),
            pltpu.VMEM((pairs, length, LANES), jnp.bfloat16),
            pltpu.SemaphoreType.DMA((3, pairs)),
            pltpu.SemaphoreType.DMA((3, pairs, n)),
            pltpu.SemaphoreType.DMA((3, pairs, n)),
            pltpu.SemaphoreType.DMA((pairs,)),
            pltpu.SemaphoreType.DMA((pairs, n)),
            pltpu.SemaphoreType.DMA((pairs, n)),
            pltpu.SemaphoreType.DMA,
            pltpu.SemaphoreType.DMA((dp_size,)),
            pltpu.SemaphoreType.DMA((dp_size,)),
            pltpu.SemaphoreType.DMA((dp_size,)),
            pltpu.SemaphoreType.DMA((dp_size,)),
        ],
        compiler_params=pltpu.CompilerParams(
            collective_id=0, has_side_effects=True, vmem_limit_bytes=40 * 1024 * 1024
        ),
        name="attention",
    )(
        queries, keys, values, decay,
        jnp.tile(query_gain, inner)[None, :], jnp.tile(key_gain, inner)[None, :],
        out_weight,
    )


def expert_kernel(
    sp_size, dp_size, per,
    send_ref, gate_ref, up_ref, down_ref,
    out_ref,
    arrived, result, gate_buf, up_buf, down_buf,
    weight_sem, send_sem, recv_sem, back_send, back_recv,
):
    n = sp_size * dp_size
    me = lax.axis_index("sp") * dp_size + lax.axis_index("dp")
    layers = 4 if sp_size % 4 == 0 else 1
    plane = n // layers
    layer, seat = me // plane, me % plane

    def partner(step, sign):
        group, turn = step // plane, step % plane
        high = (layer // 2 + 1 - group // 2) % 2
        low = (layer + (group + 1) // 2) % 2
        other = 2 * high + low if layers == 4 else layer
        return other * plane + (seat + plane + sign * turn) % plane

    cap, width = send_ref.shape[1], send_ref.shape[2]
    loads = [
        pltpu.make_async_copy(source, target, weight_sem.at[index])
        for index, (source, target) in enumerate(
            ((gate_ref, gate_buf), (up_ref, up_buf), (down_ref, down_buf))
        )
    ]
    for load in loads:
        load.start()

    def coords(flat):
        return {"sp": flat // dp_size, "dp": flat % dp_size}

    barrier = pltpu.get_barrier_semaphore()

    def greet(step, carry):
        pl.semaphore_signal(
            barrier, inc=1, device_id=coords((me + step) % n), device_id_type=MESH
        )
        return carry

    lax.fori_loop(1, n, greet, 0)
    pl.semaphore_wait(barrier, n - 1)

    def outgoing(step):
        target = partner(step, 1)
        return pltpu.make_async_remote_copy(
            src_ref=send_ref.at[target],
            dst_ref=arrived.at[step],
            send_sem=send_sem.at[step],
            recv_sem=recv_sem.at[step],
            device_id=coords(target),
            device_id_type=MESH,
        )

    def backward(step):
        target = partner(step, -1)
        return pltpu.make_async_remote_copy(
            src_ref=result.at[step],
            dst_ref=out_ref.at[me],
            send_sem=back_send.at[step],
            recv_sem=back_recv.at[step],
            device_id=coords(target),
            device_id_type=MESH,
        )

    mine = n - plane
    own = pltpu.make_async_copy(send_ref.at[me], arrived.at[mine], recv_sem.at[mine])
    own_back = pltpu.make_async_copy(result.at[mine], out_ref.at[me], back_recv.at[mine])

    def launch(step, carry):
        outgoing(step).start()
        return carry

    lax.fori_loop(0, mine, launch, 0)
    lax.fori_loop(mine + 1, n, launch, 0)
    own.start()
    for load in loads:
        load.wait()

    def chunk(index, carry):
        first = index * per
        for offset in range(per):
            if offset == 0:
                @pl.when(first == mine)
                def _():
                    own.wait()

                @pl.when(first != mine)
                def _():
                    outgoing(first).wait_recv()
            else:
                outgoing(first + offset).wait_recv()
        rows = arrived[pl.ds(first, per)].reshape(per * cap, width)
        gate = jnp.dot(rows, gate_buf[...], preferred_element_type=jnp.float32)
        upper = jnp.dot(rows, up_buf[...], preferred_element_type=jnp.float32)
        hidden = (gate / (1.0 + jnp.exp(-gate)) * upper).astype(jnp.bfloat16)
        product = jnp.dot(hidden, down_buf[...], preferred_element_type=jnp.float32)
        result[pl.ds(first, per)] = product.astype(jnp.bfloat16).reshape(per, cap, width)
        for offset in range(per):
            if offset == 0:
                @pl.when(first == mine)
                def _():
                    own_back.start()

                @pl.when(first != mine)
                def _():
                    backward(first).start()
            else:
                backward(first + offset).start()
        return carry

    lax.fori_loop(0, n // per, chunk, 0)

    def finish(step, carry):
        outgoing(step).wait_send()
        backward(step).wait()
        return carry

    own_back.wait()
    lax.fori_loop(0, mine, finish, 0)
    lax.fori_loop(mine + 1, n, finish, 0)


def run_experts(send, gate, upper, down):
    n, cap, width = send.shape
    sp_size, dp_size = lax.axis_size("sp"), lax.axis_size("dp")
    per = max(1, min(n, LANES // cap))
    return pl.pallas_call(
        functools.partial(expert_kernel, sp_size, dp_size, per),
        out_shape=jax.ShapeDtypeStruct(send.shape, jnp.bfloat16),
        in_specs=[pl.BlockSpec(memory_space=pltpu.VMEM)]
        + [pl.BlockSpec(memory_space=pl.ANY)] * 3,
        out_specs=pl.BlockSpec(memory_space=pltpu.VMEM),
        scratch_shapes=[
            pltpu.VMEM(send.shape, jnp.bfloat16),
            pltpu.VMEM(send.shape, jnp.bfloat16),
            pltpu.VMEM(gate.shape, jnp.bfloat16),
            pltpu.VMEM(upper.shape, jnp.bfloat16),
            pltpu.VMEM(down.shape, jnp.bfloat16),
            pltpu.SemaphoreType.DMA((3,)),
            pltpu.SemaphoreType.DMA((n,)),
            pltpu.SemaphoreType.DMA((n,)),
            pltpu.SemaphoreType.DMA((n,)),
            pltpu.SemaphoreType.DMA((n,)),
        ],
        compiler_params=pltpu.CompilerParams(
            collective_id=1, has_side_effects=True, vmem_limit_bytes=56 * 1024 * 1024
        ),
        name="experts",
    )(send, gate, upper, down)


def shards(
    resid,
    queries,
    keys,
    values,
    forget_cache,
    query_gain,
    key_gain,
    out_weight,
    norm_gain,
    routes,
    group_weight,
    inner_share,
    expert_gate,
    expert_up,
    expert_down,
):
    projected = exchange_attention(
        queries[0], keys[0], values[0], forget_cache[0], query_gain, key_gain, out_weight
    )
    mid = (resid[0].astype(jnp.float32) + projected).astype(jnp.bfloat16)
    normed = norm_rows(mid, norm_gain)
    width = normed.shape[1]
    tok_count = normed.shape[0]
    top_count = routes.shape[2]
    experts = lax.axis_size("sp") * lax.axis_size("dp")
    capacity = 2 * tok_count * top_count // experts
    expert_ids = routes[0].reshape(-1)
    expert_onehot = (expert_ids[:, None] == jnp.arange(experts, dtype=jnp.int32)[None, :]).astype(
        jnp.int32
    )
    earlier = jnp.cumsum(expert_onehot, axis=0) - expert_onehot
    slot_rank = jnp.sum(earlier * expert_onehot, axis=1)
    slot_index = (expert_ids * capacity + slot_rank).reshape(tok_count, top_count)
    slot_range = jnp.arange(experts * capacity, dtype=jnp.int32)
    dispatch = jnp.any(slot_range[:, None, None] == slot_index[None, :, :], axis=2).astype(
        jnp.bfloat16
    )
    send = jnp.dot(dispatch, normed, preferred_element_type=jnp.float32).astype(jnp.bfloat16)
    returned = run_experts(
        send.reshape(experts, capacity, width), expert_gate[0], expert_up[0], expert_down[0]
    )
    returned = returned.reshape(experts * capacity, width)
    shares = inner_share[0]
    weights = group_weight[0][:, None] * shares / jnp.sum(shares, axis=-1, keepdims=True)
    mixed = jnp.zeros((tok_count, width), jnp.float32)
    for route in range(top_count):
        select = (slot_range[None, :] == slot_index[:, route : route + 1]).astype(jnp.bfloat16)
        picked = jnp.dot(select, returned, preferred_element_type=jnp.float32)
        mixed = mixed + weights[:, route : route + 1] * picked
    layer_out = (mid.astype(jnp.float32) + mixed).astype(jnp.bfloat16)
    return layer_out.reshape(1, tok_count, width)


def solution(mesh):
    return jax.shard_map(
        shards,
        mesh=mesh,
        in_specs=(
            P("dp", "sp", None),
            P("dp", "sp", None),
            P("dp", "sp", None),
            P("dp", "sp", None),
            P("dp", "sp", None),
            P(),
            P(),
            P(None, "dp"),
            P(),
            P("dp", "sp", None),
            P("dp", "sp"),
            P("dp", "sp", None),
            P(("sp", "dp"), None, None),
            P(("sp", "dp"), None, None),
            P(("sp", "dp"), None, None),
        ),
        out_specs=P("dp", "sp", None),
        check_vma=False,
    )
```
